32 devices in a mesh: ep: 4 (over z), tp: 8 (over y, x, core).
Axes of the slice: x: 2, y: 2, z: 4, core: 2. Of those that a mesh axis runs over, the one named last changes fastest.
Arguments:
- tokens: bfloat16 [512, 2048], P('ep', 'tp'), may hold values from -6 to 6
- routes: int32 [512, 2], P('ep'), may hold values from 0 to 3, as said below
- route_weights: float32 [512, 2], P('ep'), may hold values from 0.1 to 1
- grad_out: bfloat16 [512, 2048], P('ep', 'tp'), may hold values from -6 to 6
- w_gate: bfloat16 [4, 2048, 2048], P('ep', 'tp'), may hold values from -0.125 to 0.125
- w_up: bfloat16 [4, 2048, 2048], P('ep', 'tp'), may hold values from -0.125 to 0.125
- w_down: bfloat16 [4, 2048, 2048], P('ep', 'tp')
Outputs:
- grad_tokens: bfloat16 [512, 2048], P('ep', 'tp')
- grad_route: float32 [512, 2], P('ep')
- grad_gate: float32 [4, 2048, 2048], P('ep', 'tp')
- grad_up: float32 [4, 2048, 2048], P('ep', 'tp')
- grad_down: float32 [4, 2048, 2048], P('ep', 'tp')
- gate_row_norms: float32 [4, 2048], P('ep')
- up_row_norms: float32 [4, 2048], P('ep')
- down_row_norms: float32 [4, 2048], P('ep', 'tp')
The draws below stay inside these ranges and needn't reach their ends.
Inputs may be any that keep to these rules, and one draw needn't show every extreme that they name: `routes`: each token names two different experts of one group: group g holds experts g * 4 to g * 4 + 3. Among the 128 rows of one device along ep no expert is named more than 64 times, and in every draw some expert is named exactly 64 times by the rows of every device along ep.
All inputs are finite; a program needn't handle non-finite values.
Results may differ from the reference program's by a relative error of at most 0.017.
Values may be sent and summed in bfloat16 or wider, within the bound.
A program may use at most 64 MiB of HBM per device.

```python
import jax
import jax.numpy as jnp
from jax import lax

D = 2048
FF = 2048
TOP = 2
GROUP_SIZE = 4
TOK_DEV = 128
EXPERTS = 4
TOKENS = 512
CAP = 64
N_EP = 4
N_TP = 8


def permute_four(sub_key):
    return jax.random.permutation(sub_key, GROUP_SIZE)


def draw_routes(key, part):
    group_total = EXPERTS // GROUP_SIZE
    hot_group = jax.random.randint(jax.random.fold_in(key, 11), (), 0, group_total)
    hot_count = 2 * CAP
    remaining = TOK_DEV - hot_count
    if group_total > 1:
        even_share = remaining // (group_total - 1)
        leftover = remaining % (group_total - 1)
        other_counts = even_share + (jnp.arange(group_total - 1) < leftover).astype(jnp.int32)
        by_rank = jnp.concatenate([jnp.array([hot_count], jnp.int32), other_counts.astype(jnp.int32)])
    else:
        by_rank = jnp.array([hot_count], jnp.int32)
    pair_table = jnp.array([[0, 1], [2, 3], [0, 2], [1, 3], [0, 3], [1, 2]], jnp.int32)

    def one_block(block_key):
        sub_keys = jax.random.split(block_key, 4)
        group_order = jax.random.permutation(sub_keys[0], group_total)
        first_group = group_order[0]
        group_order = jnp.where(group_order == hot_group, first_group, group_order)
        group_order = group_order.at[0].set(hot_group)
        group_counts = jnp.zeros((group_total,), jnp.int32).at[group_order].set(by_rank)
        group_ends = jnp.cumsum(group_counts)
        group_starts = group_ends - group_counts
        positions = jnp.arange(TOK_DEV, dtype=jnp.int32)
        group_of = jnp.sum((positions[:, None] >= group_ends[None, :]).astype(jnp.int32), axis=1)
        within = positions - group_starts[group_of]
        pair_rows = pair_table[within % 6]
        inner_perm = jax.vmap(permute_four)(jax.random.split(sub_keys[1], group_total))
        chosen = jnp.take_along_axis(inner_perm[group_of], pair_rows, axis=1)
        swap_bit = jax.random.randint(sub_keys[2], (TOK_DEV, 1), 0, 2)
        chosen = jnp.where(swap_bit == 1, chosen[:, ::-1], chosen)
        expert_ids = group_of[:, None] * GROUP_SIZE + chosen
        shuffle = jax.random.permutation(sub_keys[3], TOK_DEV)
        return expert_ids[shuffle]
    all_blocks = jax.vmap(one_block)(jax.random.split(jax.random.fold_in(key, 12), N_EP))
    return all_blocks.reshape(TOKENS, 2).astype(jnp.int32)


def draw_w_down(key, part):
    noise = jnp.clip(jax.random.normal(jax.random.fold_in(key, 21), (EXPERTS, FF, D), jnp.float32), -6.0, 6.0)
    ramp = 3.0 ** (jnp.arange(FF, dtype=jnp.float32) / FF)
    jitter = jnp.exp(jax.random.uniform(jax.random.fold_in(key, 23), (EXPERTS, FF, 1), jnp.float32, -0.7, 0.7))
    row_scale = ramp[None, :, None] * jitter / jnp.sqrt(jnp.mean(ramp * ramp))
    return (noise * row_scale * FF ** (-0.5)).astype(jnp.bfloat16)


def block_levels(rng, extent, cuts, low, top_value):
    def one(axis_at, shards_of):
        draws = jax.random.uniform(jax.random.fold_in(jax.random.fold_in(rng, 6), axis_at), (shards_of,), jnp.float32, low / len(cuts), top_value / len(cuts))
        return jnp.repeat(jnp.exp(draws), extent[axis_at] // shards_of).reshape((-1,) + (1,) * (len(extent) - axis_at - 1))

    level = one(*cuts[0])
    for cut in cuts[1:]:
        level = level * one(*cut)
    return level


def normal_values(own_key, shape, scale, reach, cuts=(), held_as=jnp.bfloat16):
    result = jax.random.normal(own_key, shape, jnp.float32) * scale
    if len(cuts) > 0:
        result = block_levels(own_key, shape, cuts, -0.22, 0.18) * result
    return jnp.clip(result, min=-reach, max=reach).astype(held_as)


def setup_inputs(seed: int = 0) -> dict:
    key_list = jax.random.split(jax.random.key(seed), 8)
    tokens = normal_values(key_list[0], (TOKENS, D), 1.0, 6.0, ((0, 4), (1, 8)))
    routes = draw_routes(jax.random.fold_in(key_list[7], 71), 0)
    route_weights = jnp.clip(0.1 + 0.9 * jax.random.uniform(key_list[2], (TOKENS, TOP), jnp.float32) ** block_levels(key_list[2], (TOKENS, TOP), ((0, 4),), -0.2, 0.2), 0.1, 1.0)
    grad_out = normal_values(key_list[3], (TOKENS, D), 1.0, 6.0, ((0, 4), (1, 8)))
    w_gate = normal_values(key_list[4], (EXPERTS, FF, D), D ** -0.5, 0.125, ((0, 4), (1, 8)))
    w_up = normal_values(key_list[5], (EXPERTS, FF, D), D ** -0.5, 0.125, ((0, 4), (1, 8)))
    w_down = draw_w_down(jax.random.fold_in(key_list[7], 71), 0)
    return {"tokens": tokens, "routes": routes, "route_weights": route_weights, "grad_out": grad_out, "w_gate": w_gate, "w_up": w_up, "w_down": w_down}


def silu_parts(pre_act):
    sigmoid_val = jax.nn.sigmoid(pre_act)
    return pre_act * sigmoid_val, sigmoid_val * (1.0 + pre_act * (1.0 - sigmoid_val))


def reference(tokens, routes, route_weights, grad_out, w_gate, w_up, w_down):
    token_total, model_width = tokens.shape
    hidden_width = w_gate.shape[1]
    flat_ids = routes.reshape(-1).astype(jnp.int32)
    slot_total = flat_ids.shape[0]
    one_hot = (flat_ids[:, None] == jnp.arange(EXPERTS, dtype=jnp.int32)[None, :]).astype(jnp.int32)
    blocked = one_hot.reshape(N_EP, slot_total // N_EP, EXPERTS)
    earlier = jnp.cumsum(blocked, axis=1) - blocked
    slot_ids = jnp.sum(earlier * blocked, axis=2).reshape(-1).astype(jnp.int32)
    source = (jnp.arange(slot_total, dtype=jnp.int32) // (slot_total // N_EP)).astype(jnp.int32)
    position = (source * CAP + slot_ids).astype(jnp.int32)
    index_table = jnp.full((EXPERTS, N_EP * CAP), slot_total, jnp.int32)
    index_table = index_table.at[flat_ids, position].set(jnp.arange(slot_total, dtype=jnp.int32))
    weight_flat = route_weights.reshape(-1)
    zero_row = jnp.zeros((1, model_width), jnp.bfloat16)
    token_rows = jnp.concatenate([jnp.repeat(tokens, 2, axis=0), zero_row], axis=0)
    scaled = (weight_flat[:, None] * jnp.repeat(grad_out, 2, axis=0).astype(jnp.float32)).astype(jnp.bfloat16)
    scaled_rows = jnp.concatenate([scaled, zero_row], axis=0)
    block_width = hidden_width // N_TP

    def one_expert(item):
        indices, gate_w, up_w, down_w = item
        x_rows = token_rows[indices]
        s_rows = scaled_rows[indices]
        gate = jnp.dot(x_rows, gate_w.T, preferred_element_type=jnp.float32)
        up = jnp.dot(x_rows, up_w.T, preferred_element_type=jnp.float32)
        active, slope = silu_parts(gate)
        hidden = (active * up).astype(jnp.bfloat16)
        dhid = jnp.dot(s_rows, down_w.T, preferred_element_type=jnp.float32)
        partial_value = jnp.sum(hidden.astype(jnp.float32) * dhid, axis=1)
        dgate = (dhid * up * slope).astype(jnp.bfloat16)
        dup = (dhid * active).astype(jnp.bfloat16)
        gate_grad = jnp.dot(dgate.T, x_rows, preferred_element_type=jnp.float32)
        up_grad = jnp.dot(dup.T, x_rows, preferred_element_type=jnp.float32)
        down_grad = jnp.dot(hidden.T, s_rows, preferred_element_type=jnp.float32)
        row_count = x_rows.shape[0]
        dgate_blocks = dgate.astype(jnp.float32).reshape(row_count, N_TP, block_width)
        dup_blocks = dup.astype(jnp.float32).reshape(row_count, N_TP, block_width)
        gate_blocks = gate_w.astype(jnp.float32).reshape(N_TP, block_width, model_width)
        up_blocks = up_w.astype(jnp.float32).reshape(N_TP, block_width, model_width)
        pieces = jnp.einsum('rjf,jfd->jrd', dgate_blocks, gate_blocks) + jnp.einsum('rjf,jfd->jrd', dup_blocks, up_blocks)
        rounded = lax.optimization_barrier(pieces.astype(jnp.bfloat16))
        dtok = jnp.sum(rounded.astype(jnp.float32), axis=0)
        return dtok, partial_value, gate_grad, up_grad, down_grad

    dtok_all, partial_all, grad_gate, grad_up, grad_down = lax.map(one_expert, (index_table, w_gate, w_up, w_down))
    dtok_slots = dtok_all[flat_ids, position]
    grad_tokens = jnp.sum(dtok_slots.reshape(token_total, 2, model_width), axis=1).astype(jnp.bfloat16)
    grad_route = (partial_all[flat_ids, position] / weight_flat).reshape(token_total, 2)
    gate_row_norms = jnp.sum(grad_gate * grad_gate, axis=1)
    up_row_norms = jnp.sum(grad_up * grad_up, axis=1)
    down_row_norms = jnp.sum(grad_down * grad_down, axis=2)
    return (grad_tokens, grad_route, grad_gate, grad_up, grad_down, gate_row_norms, up_row_norms, down_row_norms)
```

```python
import functools

import jax
import jax.numpy as jnp
from jax import lax
from jax.experimental import pallas as pl
from jax.experimental.pallas import tpu as pltpu
from jax.sharding import PartitionSpec as P

MESH = pl.DeviceIdType.MESH
F32 = jnp.float32
BF16 = jnp.bfloat16
NT = (((1,), (1,)), ((), ()))
VMEM = pl.BlockSpec(memory_space=pltpu.VMEM)
ANY = pl.BlockSpec(memory_space=pl.ANY)


def peers(j):
    core, x, y = j % 2, (j // 2) % 2, j // 4
    partner = j + 1 - 2 * core
    xnb = j + 2 - 4 * x
    ynb = j + 4 - 8 * y
    diag = xnb + 4 - 8 * y
    return partner, xnb, ynb, diag


def routing(routes_ref):
    token_count = routes_ref.shape[1]
    r0, r1 = routes_ref[0:1, :], routes_ref[1:2, :]
    eid = lax.broadcasted_iota(jnp.int32, (8, token_count), 0)
    m0, m1 = eid == r0, eid == r1
    m = jnp.logical_or(m0, m1)
    upper = (
        lax.broadcasted_iota(jnp.int32, (token_count, token_count), 0)
        < lax.broadcasted_iota(jnp.int32, (token_count, token_count), 1)
    )
    earlier = jnp.dot(
        jnp.where(m, 1.0, 0.0).astype(BF16),
        jnp.where(upper, 1.0, 0.0).astype(BF16),
        preferred_element_type=F32,
    )
    slot = jnp.where(m, earlier, -1.0)
    return m0, m1, slot


def slot_mask(slot, e, capacity):
    token_count = slot.shape[1]
    ids = lax.broadcasted_iota(jnp.int32, (capacity, token_count), 0).astype(F32)
    return slot[e : e + 1, :] == ids


def signal_all(barrier, devices):
    for device in devices:
        pl.semaphore_signal(barrier, inc=1, device_id=device, device_id_type=MESH)


def remote(src, dst, send_sem, recv_sem, device):
    return pltpu.make_async_remote_copy(
        src_ref=src,
        dst_ref=dst,
        send_sem=send_sem,
        recv_sem=recv_sem,
        device_id=device,
        device_id_type=MESH,
    )


def dispatch_kernel(
    n_ep, capacity, routes_ref, weights_ref, tok_ref, go_ref, full_ref, send_buf, zs, zr, ts, tr
):
    i, j = lax.axis_index("ep"), lax.axis_index("tp")
    width = tok_ref.shape[1]
    partner, xnb, ynb, diag = peers(j)
    barrier = pltpu.get_barrier_semaphore()
    greet = [(lax.rem(i + d, n_ep), j) for d in range(1, n_ep)]
    greet += [(i, t) for t in (partner, xnb, ynb, diag)]
    signal_all(barrier, greet)

    m0, m1, slot = routing(routes_ref)
    weight = jnp.where(m0, weights_ref[0:1, :], 0.0) + jnp.where(m1, weights_ref[1:2, :], 0.0)
    for e in range(n_ep):
        mask = slot_mask(slot, e, capacity)
        pick = jnp.where(mask, 1.0, 0.0).astype(BF16)
        rows = jnp.dot(pick, tok_ref[...], preferred_element_type=F32)
        grads = jnp.dot(pick, go_ref[...], preferred_element_type=F32)
        scale = jnp.sum(jnp.where(mask, weight[e : e + 1, :], 0.0), axis=1, keepdims=True)
        send_buf[e, 0] = rows.astype(BF16)
        send_buf[e, 1] = (grads * scale).astype(BF16)

    def area(src, col):
        return full_ref.at[
            :,
            pl.ds(pl.multiple_of(src * capacity, capacity), capacity),
            pl.ds(pl.multiple_of(col * width, width), width),
        ]

    area(i, j)[...] = send_buf[i]
    pl.semaphore_wait(barrier, len(greet))

    z_copies = {}
    for d in [2, 1, 3]:
        e = lax.rem(i + d, n_ep)
        z_copies[d] = remote(send_buf.at[e], area(i, j), zs.at[d], zr.at[d], (e, j))
        z_copies[d].start()

    order = [0, 1, 3, 2]
    copies = []
    heard = {}
    for step in range(len(order) + 1):
        if step < len(order):
            d = order[step]
            src = lax.rem(i + n_ep - d, n_ep)
            if d > 0:
                z_copies[d].wait_recv()
            mine = area(src, j) if d > 0 else send_buf.at[i]
            for kind, target in enumerate((diag, xnb, ynb, partner)):
                copy = remote(
                    mine, area(src, j), ts.at[kind, d], tr.at[kind, d], (i, target)
                )
                copy.start()
                copies.append(copy)
                heard[kind, d] = copy
        if step > 0:
            d = order[step - 1]
            src = lax.rem(i + n_ep - d, n_ep)
            for kind, owner in ((1, xnb), (2, ynb), (0, diag)):
                heard[kind, d].wait_recv()
                got = area(src, owner)
                copy = remote(got, got, ts.at[4 + kind, d], tr.at[4 + kind, d], (i, partner))
                copy.start()
                copies.append(copy)
                heard[4 + kind, d] = copy
    for d in order:
        for kind in (3, 4, 5, 6):
            heard[kind, d].wait_recv()
    for d in range(1, n_ep):
        z_copies[d].wait_send()
    for copy in copies:
        copy.wait_send()


def expert_kernel(
    n_ep, capacity, full_hbm, wg_hbm, wu_hbm, wd_hbm,
    gg_hbm, gu_hbm, gd_hbm, back_ref, small_ref, dn_ref,
    full, wg, wu, wd, gg, gu, gd, in_sem, out_sem,
):
    loads = []
    for index, (src, dst) in enumerate(
        ((full_hbm, full), (wg_hbm, wg), (wu_hbm, wu), (wd_hbm, wd))
    ):
        load = pltpu.make_async_copy(src, dst, in_sem.at[index])
        load.start()
        loads.append(load)
    hidden_dev, model_width = wg.shape
    loads[0].wait()
    loads[1].wait()
    x, s = full[0], full[1]
    gate = lax.dot_general(x, wg[...], NT, preferred_element_type=F32)
    loads[2].wait()
    up = lax.dot_general(x, wu[...], NT, preferred_element_type=F32)
    loads[3].wait()
    dhid = lax.dot_general(s, wd[...], NT, preferred_element_type=F32)
    sig = 1.0 / (1.0 + jnp.exp(-gate))
    active = gate * sig
    slope = sig * (1.0 + gate * (1.0 - sig))
    hidden_f = (active * up).astype(BF16).astype(F32)
    dgate_f = dhid * up * slope
    dup_f = dhid * active
    dgate, dup = dgate_f.astype(BF16), dup_f.astype(BF16)
    route_terms = hidden_f * dhid
    small_ref[...] = jnp.zeros_like(small_ref)
    rows_norm = model_width // 128
    for e in range(n_ep):
        block = route_terms[e * capacity : (e + 1) * capacity, :]
        small_ref[2 * rows_norm + e : 2 * rows_norm + e + 1, 0:capacity] = jnp.sum(
            block.T, axis=0, keepdims=True
        )
    dgate_t = dgate_f.T.astype(BF16)
    dup_t = dup_f.T.astype(BF16)
    hidden_t = hidden_f.T.astype(BF16)
    tile = 512
    stores = []
    down_sums = jnp.zeros((hidden_dev, 128), F32)
    for n in range(model_width // tile):
        cols = slice(n * tile, (n + 1) * tile)
        for index, (lhs, rhs, buf, out) in enumerate(
            ((dgate_t, 0, gg, gg_hbm), (dup_t, 0, gu, gu_hbm), (hidden_t, 1, gd, gd_hbm))
        ):
            grad = jnp.dot(lhs, full[rhs, :, cols], preferred_element_type=F32)
            buf[:, cols] = grad
            store = pltpu.make_async_copy(
                buf.at[:, cols], out.at[:, cols], out_sem.at[index, n]
            )
            store.start()
            stores.append(store)
            square = grad * grad
            if index < 2:
                norm = jnp.sum(square, axis=0, keepdims=True)
                for q in range(tile // 128):
                    row = index * rows_norm + n * (tile // 128) + q
                    small_ref[row : row + 1, :] = norm[:, q * 128 : (q + 1) * 128]
            else:
                for q in range(tile // 128):
                    down_sums = down_sums + square[:, q * 128 : (q + 1) * 128]
    dn_ref[...] = jnp.sum(down_sums.T, axis=0, keepdims=True)
    for n in range(model_width // tile):
        cols = slice(n * tile, (n + 1) * tile)
        back_ref[:, cols] = (
            jnp.dot(dgate, wg[:, cols], preferred_element_type=F32)
            + jnp.dot(dup, wu[:, cols], preferred_element_type=F32)
        ).astype(BF16)
    for store in stores:
        store.wait()


def combine_kernel(
    n_ep, n_tp, capacity, routes_ref, weights_ref, back_ref, small_ref,
    gt_ref, gr_ref, gn_ref, un_ref,
    pair_in, chip_sum, plane_in, z_out, z_in, small_in, route_out, route_in,
    ps, pr, cs, cr, zs, zr, ss, sr, rs, rr,
):
    i, j = lax.axis_index("ep"), lax.axis_index("tp")
    width = gt_ref.shape[1]
    n_chip = n_tp // 2
    core = j % 2
    partner, xnb, ynb, diag = peers(j)
    barrier = pltpu.get_barrier_semaphore()
    greet = [(lax.rem(i + d, n_ep), j) for d in range(1, n_ep)]
    greet += [(i, lax.rem(j + d, n_tp)) for d in range(1, n_tp)]
    signal_all(barrier, greet)
    m0, m1, slot = routing(routes_ref)
    pl.semaphore_wait(barrier, len(greet))

    order = [2, 1, 3, 0]

    def rows_of(d):
        e = lax.rem(i + d, n_ep)
        return pl.ds(pl.multiple_of(e * capacity, capacity), capacity)

    def cols_of(t):
        return pl.ds(pl.multiple_of(t * width, width), width)

    pair = {}
    for d in order:
        for q in range(n_chip):
            copy = remote(
                back_ref.at[rows_of(d), cols_of(2 * q + 1 - core)],
                pair_in.at[d, q],
                ps.at[d, q],
                pr.at[d, q],
                (i, partner),
            )
            copy.start()
            pair[d, q] = copy
    small = []
    for d in range(1, n_tp):
        copy = remote(
            small_ref, small_in.at[d - 1], ss.at[d - 1], sr.at[d - 1], (i, lax.rem(j + d, n_tp))
        )
        copy.start()
        small.append(copy)

    plane = {}
    for d in order:
        for q in range(n_chip):
            pair[d, q].wait_recv()
            mine = back_ref[rows_of(d), cols_of(2 * q + core)].astype(F32)
            chip_sum[d, q] = (mine + pair_in[d, q].astype(F32)).astype(BF16)
        for kind, target in enumerate((diag, xnb, ynb)):
            copy = remote(
                chip_sum.at[d, target // 2],
                plane_in.at[d, kind],
                cs.at[d, kind],
                cr.at[d, kind],
                (i, target),
            )
            copy.start()
            plane[d, kind] = copy

    total = small_ref[...]
    for copy in small:
        copy.wait_recv()
    for d in range(1, n_tp):
        total = total + small_in[d - 1]
    rows_norm = gn_ref.shape[1] // 128
    for r in range(rows_norm):
        gn_ref[:, r * 128 : (r + 1) * 128] = total[r : r + 1, :]
        un_ref[:, r * 128 : (r + 1) * 128] = total[rows_norm + r : rows_norm + r + 1, :]
    route_out[...] = total[2 * rows_norm : 2 * rows_norm + 8, :]
    route_in[i] = total[2 * rows_norm : 2 * rows_norm + 8, :]
    route = []
    for d in range(1, n_ep):
        copy = remote(
            route_out, route_in.at[i], rs.at[d], rr.at[d], (lax.rem(i + d, n_ep), j)
        )
        copy.start()
        route.append(copy)

    z_copies = []
    for d in order:
        for kind in range(3):
            plane[d, kind].wait_recv()
        done = (
            chip_sum[d, j // 2].astype(F32)
            + plane_in[d, 0].astype(F32)
            + plane_in[d, 1].astype(F32)
            + plane_in[d, 2].astype(F32)
        ).astype(BF16)
        if d == 0:
            z_in[i] = done
        else:
            z_out[d] = done
            copy = remote(
                z_out.at[d], z_in.at[i], zs.at[d], zr.at[d], (lax.rem(i + d, n_ep), j)
            )
            copy.start()
            z_copies.append(copy)

    for copy in route:
        copy.wait_recv()
    masks = []
    back_route = []
    for e in range(n_ep):
        pick = jnp.where(slot_mask(slot, e, capacity), 1.0, 0.0)
        masks.append(pick)
        values = route_in[e, pl.ds(i, 1), :][:, 0:capacity]
        back_route.append(
            jnp.dot(
                values, pick, preferred_element_type=F32, precision=lax.Precision.HIGHEST
            )
        )
    for k, m in enumerate((m0, m1)):
        value = jnp.zeros_like(back_route[0])
        for e in range(n_ep):
            value = value + jnp.where(m[e : e + 1, :], back_route[e], 0.0)
        gr_ref[k : k + 1, :] = value / weights_ref[k : k + 1, :]

    for copy in z_copies:
        copy.wait_recv()
    acc = jnp.zeros(gt_ref.shape, F32)
    for e in range(n_ep):
        acc = acc + jnp.dot(masks[e].T.astype(BF16), z_in[e], preferred_element_type=F32)
    gt_ref[...] = acc.astype(BF16)
    for copy in (*pair.values(), *small, *plane.values(), *route, *z_copies):
        copy.wait_send()


def per_device_kernels(tokens, routes, route_weights, grad_out, w_gate, w_up, w_down):
    token_count, width = tokens.shape
    _, hidden_dev, model_width = w_gate.shape
    n_ep, n_tp = lax.axis_size("ep"), lax.axis_size("tp")
    capacity = min(3 * token_count // n_ep, token_count // 2)
    rows = n_ep * capacity
    routes_t, weights_t = routes.T, route_weights.T
    dma = pltpu.SemaphoreType.DMA
    full = pl.pallas_call(
        functools.partial(dispatch_kernel, n_ep, capacity),
        name="dispatch",
        out_shape=jax.ShapeDtypeStruct((2, rows, model_width), BF16),
        in_specs=[VMEM] * 4,
        out_specs=VMEM,
        scratch_shapes=[
            pltpu.VMEM((n_ep, 2, capacity, width), BF16),
            dma((n_ep,)),
            dma((n_ep,)),
            dma((7, n_ep)),
            dma((7, n_ep)),
        ],
        compiler_params=pltpu.CompilerParams(collective_id=0, has_side_effects=True),
    )(routes_t, weights_t, tokens, grad_out)

    small_rows = 2 * (model_width // 128) + 8
    grad_shape = jax.ShapeDtypeStruct((hidden_dev, model_width), F32)
    grad_gate, grad_up, grad_down, back, small, down_norms = pl.pallas_call(
        functools.partial(expert_kernel, n_ep, capacity),
        name="expert",
        out_shape=(
            grad_shape,
            grad_shape,
            grad_shape,
            jax.ShapeDtypeStruct((rows, model_width), BF16),
            jax.ShapeDtypeStruct((small_rows, 128), F32),
            jax.ShapeDtypeStruct((1, hidden_dev), F32),
        ),
        in_specs=[ANY] * 4,
        out_specs=(ANY, ANY, ANY, VMEM, VMEM, VMEM),
        scratch_shapes=[
            pltpu.VMEM((2, rows, model_width), BF16),
            *[pltpu.VMEM((hidden_dev, model_width), BF16)] * 3,
            *[pltpu.VMEM((hidden_dev, model_width), F32)] * 3,
            dma((4,)),
            dma((3, model_width // 512)),
        ],
    )(full, w_gate[0], w_up[0], w_down[0])

    block = (capacity, width)
    n_chip = n_tp // 2
    grad_tokens, grad_route, gate_norms, up_norms = pl.pallas_call(
        functools.partial(combine_kernel, n_ep, n_tp, capacity),
        name="combine",
        out_shape=(
            jax.ShapeDtypeStruct((token_count, width), BF16),
            jax.ShapeDtypeStruct((2, token_count), F32),
            jax.ShapeDtypeStruct((1, model_width), F32),
            jax.ShapeDtypeStruct((1, model_width), F32),
        ),
        in_specs=[VMEM] * 4,
        out_specs=(VMEM,) * 4,
        scratch_shapes=[
            pltpu.VMEM((n_ep, n_chip, *block), BF16),
            pltpu.VMEM((n_ep, n_chip, *block), BF16),
            pltpu.VMEM((n_ep, 3, *block), BF16),
            pltpu.VMEM((n_ep, *block), BF16),
            pltpu.VMEM((n_ep, *block), BF16),
            pltpu.VMEM((n_tp - 1, small_rows, 128), F32),
            pltpu.VMEM((8, 128), F32),
            pltpu.VMEM((n_ep, 8, 128), F32),
            dma((n_ep, n_chip)),
            dma((n_ep, n_chip)),
            dma((n_ep, 3)),
            dma((n_ep, 3)),
            dma((n_ep,)),
            dma((n_ep,)),
            dma((n_tp - 1,)),
            dma((n_tp - 1,)),
            dma((n_ep,)),
            dma((n_ep,)),
        ],
        compiler_params=pltpu.CompilerParams(collective_id=1, has_side_effects=True),
    )(routes_t, weights_t, back, small)
    return (
        grad_tokens,
        grad_route.T,
        grad_gate[None],
        grad_up[None],
        grad_down[None],
        gate_norms,
        up_norms,
        down_norms,
    )


def silu_parts(pre_act):
    sigmoid_val = jax.nn.sigmoid(pre_act)
    return (pre_act * sigmoid_val, sigmoid_val * (1.0 + pre_act * (1.0 - sigmoid_val)))


def per_device(tokens, routes, route_weights, grad_out, w_gate, w_up, w_down):
    token_count, feature_dev = tokens.shape
    experts_dev, hidden_dev, model_width = w_gate.shape
    ep_size = lax.axis_size("ep")
    expert_total = experts_dev * ep_size
    capacity = min(3 * token_count // expert_total, token_count // 2)
    slot_count = expert_total * capacity
    row_count = ep_size * capacity
    flat_ids = routes.reshape(-1)
    pair_count = flat_ids.shape[0]
    one_hot = (flat_ids[:, None] == jnp.arange(expert_total, dtype=jnp.int32)[None, :]).astype(
        jnp.bfloat16
    )
    lower = (
        jnp.arange(pair_count, dtype=jnp.int32)[:, None]
        > jnp.arange(pair_count, dtype=jnp.int32)[None, :]
    ).astype(jnp.bfloat16)
    earlier = jnp.dot(lower, one_hot, preferred_element_type=jnp.float32)
    slot_ids = jnp.sum(earlier * one_hot.astype(jnp.float32), axis=1).astype(jnp.int32)
    position = flat_ids % experts_dev * row_count + flat_ids // experts_dev * capacity + slot_ids
    dispatch = (position[None, :] == jnp.arange(slot_count, dtype=jnp.int32)[:, None]).astype(
        jnp.bfloat16
    )
    weight_flat = route_weights.reshape(-1)
    token_rows = jnp.repeat(tokens, 2, axis=0)
    scaled = (weight_flat[:, None] * jnp.repeat(grad_out, 2, axis=0).astype(jnp.float32)).astype(
        jnp.bfloat16
    )
    send_shape = (experts_dev, ep_size, capacity, feature_dev)
    x_send = (
        jnp.dot(dispatch, token_rows, preferred_element_type=jnp.float32)
        .astype(jnp.bfloat16)
        .reshape(send_shape)
    )
    s_send = (
        jnp.dot(dispatch, scaled, preferred_element_type=jnp.float32)
        .astype(jnp.bfloat16)
        .reshape(send_shape)
    )
    x_recv, s_recv = (
        lax.all_to_all(x_send, "ep", split_axis=1, concat_axis=1, tiled=True),
        lax.all_to_all(s_send, "ep", split_axis=1, concat_axis=1, tiled=True),
    )
    x_full, s_full = (
        lax.all_gather(x_recv, "tp", axis=3, tiled=True),
        lax.all_gather(s_recv, "tp", axis=3, tiled=True),
    )
    x_rows = x_full.reshape(experts_dev, row_count, model_width)
    s_rows = s_full.reshape(experts_dev, row_count, model_width)
    gate = jnp.einsum("erd,efd->erf", x_rows, w_gate, preferred_element_type=jnp.float32)
    up = jnp.einsum("erd,efd->erf", x_rows, w_up, preferred_element_type=jnp.float32)
    dhid = jnp.einsum("erd,efd->erf", s_rows, w_down, preferred_element_type=jnp.float32)
    active, slope = silu_parts(gate)
    hidden = (active * up).astype(jnp.bfloat16)
    partial_value = jnp.sum(hidden.astype(jnp.float32) * dhid, axis=2)
    dgate = (dhid * up * slope).astype(jnp.bfloat16)
    dup = (dhid * active).astype(jnp.bfloat16)
    grad_gate = jnp.einsum("erf,erd->efd", dgate, x_rows, preferred_element_type=jnp.float32)
    grad_up = jnp.einsum("erf,erd->efd", dup, x_rows, preferred_element_type=jnp.float32)
    grad_down = jnp.einsum("erf,erd->efd", hidden, s_rows, preferred_element_type=jnp.float32)
    back_terms = jnp.einsum("erf,efd->erd", dgate, w_gate, preferred_element_type=jnp.float32)
    back_terms = back_terms + jnp.einsum(
        "erf,efd->erd", dup, w_up, preferred_element_type=jnp.float32
    )
    back_terms = back_terms.reshape(experts_dev, ep_size, capacity, model_width)
    gate_norms = jnp.sum(grad_gate * grad_gate, axis=1)
    up_norms = jnp.sum(grad_up * grad_up, axis=1)
    down_norms = jnp.sum(grad_down * grad_down, axis=2)
    partial_value, gate_norms, up_norms = lax.psum((partial_value, gate_norms, up_norms), "tp")
    partial_sent = partial_value.reshape(experts_dev, ep_size, capacity)
    dtok_mine = lax.psum_scatter(
        back_terms.astype(jnp.bfloat16), "tp", scatter_dimension=3, tiled=True
    ).astype(jnp.float32)
    returned, partial_back = (
        lax.all_to_all(
            dtok_mine.astype(jnp.bfloat16), "ep", split_axis=1, concat_axis=1, tiled=True
        ).astype(dtok_mine.dtype),
        lax.all_to_all(
            partial_sent.astype(jnp.bfloat16), "ep", split_axis=1, concat_axis=1, tiled=True
        ).astype(partial_sent.dtype),
    )
    slot_rows = jnp.take(returned.reshape(slot_count, feature_dev), position, axis=0)
    grad_tokens = jnp.sum(slot_rows.reshape(token_count, 2, feature_dev), axis=1).astype(
        jnp.bfloat16
    )
    slot_partial = jnp.take(partial_back.reshape(slot_count), position, axis=0)
    grad_route = (slot_partial / weight_flat).reshape(token_count, 2)
    return (
        grad_tokens,
        grad_route,
        grad_gate,
        grad_up,
        grad_down,
        gate_norms,
        up_norms,
        down_norms,
    )


def solution(mesh):
    in_specs = (
        P("ep", "tp"),
        P("ep", None),
        P("ep", None),
        P("ep", "tp"),
        P("ep", "tp", None),
        P("ep", "tp", None),
        P("ep", "tp", None),
    )
    out_specs = (
        P("ep", "tp"),
        P("ep", None),
        P("ep", "tp", None),
        P("ep", "tp", None),
        P("ep", "tp", None),
        P("ep", None),
        P("ep", None),
        P("ep", "tp"),
    )
    fits = mesh.shape["tp"] == 8 and mesh.shape["ep"] == 4
    return jax.shard_map(
        per_device_kernels if fits else per_device, mesh=mesh, in_specs=in_specs, out_specs=out_specs, check_vma=False
    )
```

```python
import functools

import jax
import jax.numpy as jnp
from jax import lax
from jax.experimental import pallas as pl
from jax.experimental.pallas import tpu as pltpu
from jax.sharding import PartitionSpec as P

MESH = pl.DeviceIdType.MESH
F32 = jnp.float32
BF16 = jnp.bfloat16
NT = (((1,), (1,)), ((), ()))
VMEM = pl.BlockSpec(memory_space=pltpu.VMEM)
ANY = pl.BlockSpec(memory_space=pl.ANY)


def peers(j):
    core, x, y = j % 2, (j // 2) % 2, j // 4
    partner = j + 1 - 2 * core
    xnb = j + 2 - 4 * x
    ynb = j + 4 - 8 * y
    diag = xnb + 4 - 8 * y
    return partner, xnb, ynb, diag


def routing(routes_ref):
    token_count = routes_ref.shape[1]
    r0, r1 = routes_ref[0:1, :], routes_ref[1:2, :]
    eid = lax.broadcasted_iota(jnp.int32, (8, token_count), 0)
    m0, m1 = eid == r0, eid == r1
    m = jnp.logical_or(m0, m1)
    upper = (
        lax.broadcasted_iota(jnp.int32, (token_count, token_count), 0)
        < lax.broadcasted_iota(jnp.int32, (token_count, token_count), 1)
    )
    earlier = jnp.dot(
        jnp.where(m, 1.0, 0.0).astype(BF16),
        jnp.where(upper, 1.0, 0.0).astype(BF16),
        preferred_element_type=F32,
    )
    slot = jnp.where(m, earlier, -1.0)
    return m0, m1, slot


def slot_mask(slot, e, capacity):
    token_count = slot.shape[1]
    ids = lax.broadcasted_iota(jnp.int32, (capacity, token_count), 0).astype(F32)
    return slot[e : e + 1, :] == ids


def signal_all(barrier, devices):
    for device in devices:
        pl.semaphore_signal(barrier, inc=1, device_id=device, device_id_type=MESH)


def remote(src, dst, send_sem, recv_sem, device):
    return pltpu.make_async_remote_copy(
        src_ref=src,
        dst_ref=dst,
        send_sem=send_sem,
        recv_sem=recv_sem,
        device_id=device,
        device_id_type=MESH,
    )


def step_kernel(
    n_ep, n_tp, capacity, routes_ref, weights_ref, tok_ref, go_ref, wg_hbm, wu_hbm, wd_hbm,
    full_hbm, lhs_ref, z_in, route_in, norm_total,
    full, send_buf, wg, wu, wd, back, pair_in, chip_sum, plane_in, z_out,
    part_out, part_in, route_out, norm_out, norm_in,
    in_sem, zs, zr, ts, tr, ps, pr, cs, cr, qs, qr, rs, rr, ns, nr, bs, br,
):
    i, j = lax.axis_index("ep"), lax.axis_index("tp")
    width = tok_ref.shape[1]
    model_width = wg.shape[1]
    n_chip = n_tp // 2
    core = j % 2
    partner, xnb, ynb, diag = peers(j)
    barrier = pltpu.get_barrier_semaphore()
    greet = [(lax.rem(i + d, n_ep), j) for d in range(1, n_ep)]
    greet += [(i, lax.rem(j + d, n_tp)) for d in range(1, n_tp)]
    signal_all(barrier, greet)
    loads = []
    for index, (source, target) in enumerate(((wg_hbm, wg), (wu_hbm, wu), (wd_hbm, wd))):
        load = pltpu.make_async_copy(source, target, in_sem.at[index])
        load.start()
        loads.append(load)

    m0, m1, slot = routing(routes_ref)
    weight = jnp.where(m0, weights_ref[0:1, :], 0.0) + jnp.where(m1, weights_ref[1:2, :], 0.0)
    for e in range(n_ep):
        mask = slot_mask(slot, e, capacity)
        pick = jnp.where(mask, 1.0, 0.0).astype(BF16)
        rows = jnp.dot(pick, tok_ref[...], preferred_element_type=F32)
        grads = jnp.dot(pick, go_ref[...], preferred_element_type=F32)
        scale = jnp.sum(jnp.where(mask, weight[e : e + 1, :], 0.0), axis=1, keepdims=True)
        send_buf[e, 0] = rows.astype(BF16)
        send_buf[e, 1] = (grads * scale).astype(BF16)

    def rows_at(e):
        return pl.ds(pl.multiple_of(e * capacity, capacity), capacity)

    def cols_at(t):
        return pl.ds(pl.multiple_of(t * width, width), width)

    def area(src, col):
        return full.at[:, rows_at(src), cols_at(col)]

    area(i, j)[...] = send_buf[i]
    pl.semaphore_wait(barrier, len(greet))

    z_copies = {}
    for d in [2, 1, 3]:
        e = lax.rem(i + d, n_ep)
        z_copies[d] = remote(send_buf.at[e], area(i, j), zs.at[d], zr.at[d], (e, j))
        z_copies[d].start()

    copies = []
    heard = {}

    def push(kind, d, source, target, device):
        copy = remote(source, target, ts.at[kind, d], tr.at[kind, d], (i, device))
        copy.start()
        copies.append(copy)
        heard[kind, d] = copy

    order = [0, 1, 3, 2]
    for step in range(len(order) + 2):
        if step < len(order):
            d = order[step]
            src = lax.rem(i + n_ep - d, n_ep)
            if d > 0:
                z_copies[d].wait_recv()
            mine = area(src, j) if d > 0 else send_buf.at[i]
            push(0, d, mine, area(src, j), xnb)
            push(1, d, mine, area(src, j), ynb)
            push(4, d, mine, area(src, j), partner)
        if 0 < step <= len(order):
            d = order[step - 1]
            src = lax.rem(i + n_ep - d, n_ep)
            heard[0, d].wait_recv()
            half = full.at[0, rows_at(src), cols_at(xnb)]
            push(2, d, half, half, ynb)
            push(5, d, area(src, xnb), area(src, xnb), partner)
            heard[1, d].wait_recv()
            half = full.at[1, rows_at(src), cols_at(ynb)]
            push(3, d, half, half, xnb)
            push(6, d, area(src, ynb), area(src, ynb), partner)
        if step > 1:
            d = order[step - 2]
            src = lax.rem(i + n_ep - d, n_ep)
            for kind in (0, 1):
                heard[2 + kind, d].wait_recv()
                half = full.at[kind, rows_at(src), cols_at(diag)]
                push(7 + kind, d, half, half, partner)
    for d in order:
        for kind in (4, 5, 6, 7, 8):
            heard[kind, d].wait_recv()

    save = pltpu.make_async_copy(full, full_hbm, in_sem.at[3])
    save.start()
    for load in loads:
        load.wait()
    gate = lax.dot_general(full[0], wg[...], NT, preferred_element_type=F32)
    up = lax.dot_general(full[0], wu[...], NT, preferred_element_type=F32)
    dhid = lax.dot_general(full[1], wd[...], NT, preferred_element_type=F32)
    sig = 1.0 / (1.0 + jnp.exp(-gate))
    active = gate * sig
    slope = sig * (1.0 + gate * (1.0 - sig))
    hidden_f = (active * up).astype(BF16).astype(F32)
    dgate_f = dhid * up * slope
    dup_f = dhid * active
    dgate, dup = dgate_f.astype(BF16), dup_f.astype(BF16)

    ring = [2, 1, 3, 0]
    pair = {}
    for q in range(n_chip):
        cols = slice(2 * q * width, 2 * (q + 1) * width)
        back[:, cols] = (
            jnp.dot(dgate, wg[:, cols], preferred_element_type=F32)
            + jnp.dot(dup, wu[:, cols], preferred_element_type=F32)
        ).astype(BF16)
        for d in ring:
            e = lax.rem(i + d, n_ep)
            pair[d, q] = remote(
                back.at[rows_at(e), cols_at(2 * q + 1 - core)],
                pair_in.at[d, q],
                ps.at[d, q],
                pr.at[d, q],
                (i, partner),
            )
            pair[d, q].start()

    route_terms = hidden_f * dhid
    part_out[...] = jnp.zeros_like(part_out)
    for e in range(n_ep):
        block = route_terms[e * capacity : (e + 1) * capacity, :]
        part_out[e : e + 1, 0:capacity] = jnp.sum(block.T, axis=0, keepdims=True)
    part = []
    for d in range(1, n_tp):
        copy = remote(
            part_out, part_in.at[d - 1], qs.at[d - 1], qr.at[d - 1], (i, lax.rem(j + d, n_tp))
        )
        copy.start()
        part.append(copy)

    plane = {}
    for d in ring:
        e = lax.rem(i + d, n_ep)
        for q in range(n_chip):
            pair[d, q].wait_recv()
            mine = back[rows_at(e), cols_at(2 * q + core)].astype(F32)
            chip_sum[d, q] = (mine + pair_in[d, q].astype(F32)).astype(BF16)
        for kind, target in enumerate((diag, xnb, ynb)):
            plane[d, kind] = remote(
                chip_sum.at[d, target // 2],
                plane_in.at[d, kind],
                cs.at[d, kind],
                cr.at[d, kind],
                (i, target),
            )
            plane[d, kind].start()

    lhs_ref[0] = dgate_f.T.astype(BF16)
    lhs_ref[1] = dup_f.T.astype(BF16)
    lhs_ref[2] = hidden_f.T.astype(BF16)
    rows_norm = model_width // 128
    tile = 512
    for index in range(2):
        for n in range(model_width // tile):
            cols = slice(n * tile, (n + 1) * tile)
            grad = jnp.dot(lhs_ref[index], full[0, :, cols], preferred_element_type=F32)
            norm = jnp.sum(grad * grad, axis=0, keepdims=True)
            for q in range(tile // 128):
                row = index * rows_norm + n * (tile // 128) + q
                norm_out[row : row + 1, :] = norm[:, q * 128 : (q + 1) * 128]
    norms = []
    for d in range(1, n_tp):
        copy = remote(
            norm_out, norm_in.at[d - 1], ns.at[d - 1], nr.at[d - 1], (i, lax.rem(j + d, n_tp))
        )
        copy.start()
        norms.append(copy)

    for copy in part:
        copy.wait_recv()
    total = part_out[...]
    for d in range(1, n_tp):
        total = total + part_in[d - 1]
    route_out[...] = total
    route_in[i] = total
    route = []
    for d in range(1, n_ep):
        copy = remote(
            route_out, route_in.at[i], rs.at[d], rr.at[d], (lax.rem(i + d, n_ep), j)
        )
        copy.start()
        route.append(copy)

    returns = []
    for d in ring:
        for kind in range(3):
            plane[d, kind].wait_recv()
        done = (
            chip_sum[d, j // 2].astype(F32)
            + plane_in[d, 0].astype(F32)
            + plane_in[d, 1].astype(F32)
            + plane_in[d, 2].astype(F32)
        ).astype(BF16)
        if d == 0:
            z_in[i] = done
        else:
            z_out[d] = done
            copy = remote(
                z_out.at[d], z_in.at[i], bs.at[d], br.at[d], (lax.rem(i + d, n_ep), j)
            )
            copy.start()
            returns.append(copy)

    for copy in norms:
        copy.wait_recv()
    total = norm_out[...]
    for d in range(1, n_tp):
        total = total + norm_in[d - 1]
    norm_total[...] = total
    for copy in (*route, *returns):
        copy.wait_recv()
    for copy in (
        *z_copies.values(), *copies, *pair.values(), *part, *plane.values(),
        *norms, *route, *returns,
    ):
        copy.wait_send()
    save.wait()


def finish_kernel(
    n_ep, capacity, routes_ref, weights_ref, full_hbm, lhs_ref, z_in, route_in, norm_total,
    gg_hbm, gu_hbm, gd_hbm, gt_ref, gr_ref, gn_ref, un_ref, dn_ref,
    full, gg, gu, gd, in_sem, out_sem,
):
    loads = []
    for index in range(2):
        load = pltpu.make_async_copy(full_hbm.at[index], full.at[index], in_sem.at[index])
        load.start()
        loads.append(load)
    _, hidden_dev, _ = lhs_ref.shape
    model_width = full.shape[2]
    tile = 512
    stores = []
    down_sums = jnp.zeros((hidden_dev, 128), F32)
    for index, (rhs, buf, out) in enumerate(((0, gg, gg_hbm), (0, gu, gu_hbm), (1, gd, gd_hbm))):
        if index != 1:
            loads[rhs].wait()
        for n in range(model_width // tile):
            cols = slice(n * tile, (n + 1) * tile)
            grad = jnp.dot(lhs_ref[index], full[rhs, :, cols], preferred_element_type=F32)
            buf[:, cols] = grad
            store = pltpu.make_async_copy(
                buf.at[:, cols], out.at[:, cols], out_sem.at[index, n]
            )
            store.start()
            stores.append(store)
            if index == 2:
                square = grad * grad
                for q in range(tile // 128):
                    down_sums = down_sums + square[:, q * 128 : (q + 1) * 128]
    dn_ref[...] = jnp.sum(down_sums.T, axis=0, keepdims=True)
    rows_norm = model_width // 128
    for r in range(rows_norm):
        gn_ref[:, r * 128 : (r + 1) * 128] = norm_total[r : r + 1, :]
        un_ref[:, r * 128 : (r + 1) * 128] = norm_total[rows_norm + r : rows_norm + r + 1, :]

    i = lax.axis_index("ep")
    m0, m1, slot = routing(routes_ref)
    acc = jnp.zeros(gt_ref.shape, F32)
    back_route = []
    for e in range(n_ep):
        pick = jnp.where(slot_mask(slot, e, capacity), 1.0, 0.0)
        acc = acc + jnp.dot(pick.T.astype(BF16), z_in[e], preferred_element_type=F32)
        values = route_in[e, pl.ds(i, 1), :][:, 0:capacity]
        back_route.append(
            jnp.dot(
                values, pick, preferred_element_type=F32, precision=lax.Precision.HIGHEST
            )
        )
    gt_ref[...] = acc.astype(BF16)
    for k, m in enumerate((m0, m1)):
        value = jnp.zeros_like(back_route[0])
        for e in range(n_ep):
            value = value + jnp.where(m[e : e + 1, :], back_route[e], 0.0)
        gr_ref[k : k + 1, :] = value / weights_ref[k : k + 1, :]
    for store in stores:
        store.wait()


def per_device_kernels(tokens, routes, route_weights, grad_out, w_gate, w_up, w_down):
    token_count, width = tokens.shape
    _, hidden_dev, model_width = w_gate.shape
    n_ep, n_tp = lax.axis_size("ep"), lax.axis_size("tp")
    n_chip = n_tp // 2
    capacity = min(3 * token_count // n_ep, token_count // 2)
    rows = n_ep * capacity
    block = (capacity, width)
    norm_rows = 2 * (model_width // 128)
    routes_t, weights_t = routes.T, route_weights.T
    dma = pltpu.SemaphoreType.DMA
    full, lhs, z_in, route_in, norm_total = pl.pallas_call(
        functools.partial(step_kernel, n_ep, n_tp, capacity),
        name="step",
        out_shape=(
            jax.ShapeDtypeStruct((2, rows, model_width), BF16),
            jax.ShapeDtypeStruct((3, hidden_dev, rows), BF16),
            jax.ShapeDtypeStruct((n_ep, *block), BF16),
            jax.ShapeDtypeStruct((n_ep, 8, 128), F32),
            jax.ShapeDtypeStruct((norm_rows, 128), F32),
        ),
        in_specs=[VMEM] * 4 + [ANY] * 3,
        out_specs=(ANY, VMEM, VMEM, VMEM, VMEM),
        scratch_shapes=[
            pltpu.VMEM((2, rows, model_width), BF16),
            pltpu.VMEM((n_ep, 2, *block), BF16),
            *[pltpu.VMEM((hidden_dev, model_width), BF16)] * 3,
            pltpu.VMEM((rows, model_width), BF16),
            pltpu.VMEM((n_ep, n_chip, *block), BF16),
            pltpu.VMEM((n_ep, n_chip, *block), BF16),
            pltpu.VMEM((n_ep, 3, *block), BF16),
            pltpu.VMEM((n_ep, *block), BF16),
            pltpu.VMEM((8, 128), F32),
            pltpu.VMEM((n_tp - 1, 8, 128), F32),
            pltpu.VMEM((8, 128), F32),
            pltpu.VMEM((norm_rows, 128), F32),
            pltpu.VMEM((n_tp - 1, norm_rows, 128), F32),
            dma((4,)),
            *[dma((n_ep,))] * 2,
            *[dma((9, n_ep))] * 2,
            *[dma((n_ep, n_chip))] * 2,
            *[dma((n_ep, 3))] * 2,
            *[dma((n_tp - 1,))] * 2,
            *[dma((n_ep,))] * 2,
            *[dma((n_tp - 1,))] * 2,
            *[dma((n_ep,))] * 2,
        ],
        compiler_params=pltpu.CompilerParams(collective_id=0, has_side_effects=True),
    )(routes_t, weights_t, tokens, grad_out, w_gate[0], w_up[0], w_down[0])

    grad_shape = jax.ShapeDtypeStruct((hidden_dev, model_width), F32)
    norm_shape = jax.ShapeDtypeStruct((1, model_width), F32)
    grad_gate, grad_up, grad_down, grad_tokens, grad_route, gate_norms, up_norms, down_norms = (
        pl.pallas_call(
            functools.partial(finish_kernel, n_ep, capacity),
            name="finish",
            out_shape=(
                *[grad_shape] * 3,
                jax.ShapeDtypeStruct((token_count, width), BF16),
                jax.ShapeDtypeStruct((2, token_count), F32),
                *[norm_shape] * 2,
                jax.ShapeDtypeStruct((1, hidden_dev), F32),
            ),
            in_specs=[VMEM, VMEM, ANY, VMEM, VMEM, VMEM, VMEM],
            out_specs=(*[ANY] * 3, *[VMEM] * 5),
            scratch_shapes=[
                pltpu.VMEM((2, rows, model_width), BF16),
                *[pltpu.VMEM((hidden_dev, model_width), F32)] * 3,
                dma((2,)),
                dma((3, model_width // 512)),
            ],
        )(routes_t, weights_t, full, lhs, z_in, route_in, norm_total)
    )
    return (
        grad_tokens,
        grad_route.T,
        grad_gate[None],
        grad_up[None],
        grad_down[None],
        gate_norms,
        up_norms,
        down_norms,
    )


def silu_parts(pre_act):
    sigmoid_val = jax.nn.sigmoid(pre_act)
    return (pre_act * sigmoid_val, sigmoid_val * (1.0 + pre_act * (1.0 - sigmoid_val)))


def per_device(tokens, routes, route_weights, grad_out, w_gate, w_up, w_down):
    token_count, feature_dev = tokens.shape
    experts_dev, hidden_dev, model_width = w_gate.shape
    ep_size = lax.axis_size("ep")
    expert_total = experts_dev * ep_size
    capacity = min(3 * token_count // expert_total, token_count // 2)
    slot_count = expert_total * capacity
    row_count = ep_size * capacity
    flat_ids = routes.reshape(-1)
    pair_count = flat_ids.shape[0]
    one_hot = (flat_ids[:, None] == jnp.arange(expert_total, dtype=jnp.int32)[None, :]).astype(
        jnp.bfloat16
    )
    lower = (
        jnp.arange(pair_count, dtype=jnp.int32)[:, None]
        > jnp.arange(pair_count, dtype=jnp.int32)[None, :]
    ).astype(jnp.bfloat16)
    earlier = jnp.dot(lower, one_hot, preferred_element_type=jnp.float32)
    slot_ids = jnp.sum(earlier * one_hot.astype(jnp.float32), axis=1).astype(jnp.int32)
    position = flat_ids % experts_dev * row_count + flat_ids // experts_dev * capacity + slot_ids
    dispatch = (position[None, :] == jnp.arange(slot_count, dtype=jnp.int32)[:, None]).astype(
        jnp.bfloat16
    )
    weight_flat = route_weights.reshape(-1)
    token_rows = jnp.repeat(tokens, 2, axis=0)
    scaled = (weight_flat[:, None] * jnp.repeat(grad_out, 2, axis=0).astype(jnp.float32)).astype(
        jnp.bfloat16
    )
    send_shape = (experts_dev, ep_size, capacity, feature_dev)
    x_send = (
        jnp.dot(dispatch, token_rows, preferred_element_type=jnp.float32)
        .astype(jnp.bfloat16)
        .reshape(send_shape)
    )
    s_send = (
        jnp.dot(dispatch, scaled, preferred_element_type=jnp.float32)
        .astype(jnp.bfloat16)
        .reshape(send_shape)
    )
    x_recv, s_recv = (
        lax.all_to_all(x_send, "ep", split_axis=1, concat_axis=1, tiled=True),
        lax.all_to_all(s_send, "ep", split_axis=1, concat_axis=1, tiled=True),
    )
    x_full, s_full = (
        lax.all_gather(x_recv, "tp", axis=3, tiled=True),
        lax.all_gather(s_recv, "tp", axis=3, tiled=True),
    )
    x_rows = x_full.reshape(experts_dev, row_count, model_width)
    s_rows = s_full.reshape(experts_dev, row_count, model_width)
    gate = jnp.einsum("erd,efd->erf", x_rows, w_gate, preferred_element_type=jnp.float32)
    up = jnp.einsum("erd,efd->erf", x_rows, w_up, preferred_element_type=jnp.float32)
    dhid = jnp.einsum("erd,efd->erf", s_rows, w_down, preferred_element_type=jnp.float32)
    active, slope = silu_parts(gate)
    hidden = (active * up).astype(jnp.bfloat16)
    partial_value = jnp.sum(hidden.astype(jnp.float32) * dhid, axis=2)
    dgate = (dhid * up * slope).astype(jnp.bfloat16)
    dup = (dhid * active).astype(jnp.bfloat16)
    grad_gate = jnp.einsum("erf,erd->efd", dgate, x_rows, preferred_element_type=jnp.float32)
    grad_up = jnp.einsum("erf,erd->efd", dup, x_rows, preferred_element_type=jnp.float32)
    grad_down = jnp.einsum("erf,erd->efd", hidden, s_rows, preferred_element_type=jnp.float32)
    back_terms = jnp.einsum("erf,efd->erd", dgate, w_gate, preferred_element_type=jnp.float32)
    back_terms = back_terms + jnp.einsum(
        "erf,efd->erd", dup, w_up, preferred_element_type=jnp.float32
    )
    back_terms = back_terms.reshape(experts_dev, ep_size, capacity, model_width)
    gate_norms = jnp.sum(grad_gate * grad_gate, axis=1)
    up_norms = jnp.sum(grad_up * grad_up, axis=1)
    down_norms = jnp.sum(grad_down * grad_down, axis=2)
    partial_value, gate_norms, up_norms = lax.psum((partial_value, gate_norms, up_norms), "tp")
    partial_sent = partial_value.reshape(experts_dev, ep_size, capacity)
    dtok_mine = lax.psum_scatter(
        back_terms.astype(jnp.bfloat16), "tp", scatter_dimension=3, tiled=True
    ).astype(jnp.float32)
    returned, partial_back = (
        lax.all_to_all(
            dtok_mine.astype(jnp.bfloat16), "ep", split_axis=1, concat_axis=1, tiled=True
        ).astype(dtok_mine.dtype),
        lax.all_to_all(
            partial_sent.astype(jnp.bfloat16), "ep", split_axis=1, concat_axis=1, tiled=True
        ).astype(partial_sent.dtype),
    )
    slot_rows = jnp.take(returned.reshape(slot_count, feature_dev), position, axis=0)
    grad_tokens = jnp.sum(slot_rows.reshape(token_count, 2, feature_dev), axis=1).astype(
        jnp.bfloat16
    )
    slot_partial = jnp.take(partial_back.reshape(slot_count), position, axis=0)
    grad_route = (slot_partial / weight_flat).reshape(token_count, 2)
    return (
        grad_tokens,
        grad_route,
        grad_gate,
        grad_up,
        grad_down,
        gate_norms,
        up_norms,
        down_norms,
    )


def solution(mesh):
    in_specs = (
        P("ep", "tp"),
        P("ep", None),
        P("ep", None),
        P("ep", "tp"),
        P("ep", "tp", None),
        P("ep", "tp", None),
        P("ep", "tp", None),
    )
    out_specs = (
        P("ep", "tp"),
        P("ep", None),
        P("ep", "tp", None),
        P("ep", "tp", None),
        P("ep", "tp", None),
        P("ep", None),
        P("ep", None),
        P("ep", "tp"),
    )
    fits = mesh.shape["tp"] == 8 and mesh.shape["ep"] == 4
    return jax.shard_map(
        per_device_kernels if fits else per_device, mesh=mesh, in_specs=in_specs, out_specs=out_specs, check_vma=False
    )
```

```python
import functools

import jax
import jax.numpy as jnp
from jax import lax
from jax.experimental import pallas as pl
from jax.experimental.pallas import tpu as pltpu
from jax.sharding import PartitionSpec as P

MESH = pl.DeviceIdType.MESH
F32 = jnp.float32
BF16 = jnp.bfloat16
NT = (((1,), (1,)), ((), ()))
VMEM = pl.BlockSpec(memory_space=pltpu.VMEM)
ANY = pl.BlockSpec(memory_space=pl.ANY)


def peers(j):
    core, x, y = j % 2, (j // 2) % 2, j // 4
    partner = j + 1 - 2 * core
    xnb = j + 2 - 4 * x
    ynb = j + 4 - 8 * y
    diag = xnb + 4 - 8 * y
    return partner, xnb, ynb, diag


def routing(routes_ref):
    token_count = routes_ref.shape[1]
    r0, r1 = routes_ref[0:1, :], routes_ref[1:2, :]
    eid = lax.broadcasted_iota(jnp.int32, (8, token_count), 0)
    m0, m1 = eid == r0, eid == r1
    m = jnp.logical_or(m0, m1)
    upper = (
        lax.broadcasted_iota(jnp.int32, (token_count, token_count), 0)
        < lax.broadcasted_iota(jnp.int32, (token_count, token_count), 1)
    )
    earlier = jnp.dot(
        jnp.where(m, 1.0, 0.0).astype(BF16),
        jnp.where(upper, 1.0, 0.0).astype(BF16),
        preferred_element_type=F32,
    )
    slot = jnp.where(m, earlier, -1.0)
    return m0, m1, slot


def slot_mask(slot, e, capacity):
    token_count = slot.shape[1]
    ids = lax.broadcasted_iota(jnp.int32, (capacity, token_count), 0).astype(F32)
    return slot[e : e + 1, :] == ids


def signal_all(barrier, devices):
    for device in devices:
        pl.semaphore_signal(barrier, inc=1, device_id=device, device_id_type=MESH)


def remote(src, dst, send_sem, recv_sem, device):
    return pltpu.make_async_remote_copy(
        src_ref=src,
        dst_ref=dst,
        send_sem=send_sem,
        recv_sem=recv_sem,
        device_id=device,
        device_id_type=MESH,
    )


def step_kernel(
    n_ep, n_tp, capacity, routes_ref, weights_ref, tok_ref, go_ref, wg_hbm, wu_hbm, wd_hbm,
    full_hbm, lhs_ref, z_in, route_in, norm_total,
    full, send_buf, wg, wu, wd, back, pair_in, chip_sum, plane_in, z_out,
    part_out, part_in, route_out, norm_out, norm_in,
    in_sem, zs, zr, ts, tr, ps, pr, cs, cr, qs, qr, rs, rr, ns, nr, bs, br,
):
    i, j = lax.axis_index("ep"), lax.axis_index("tp")
    width = tok_ref.shape[1]
    model_width = wg.shape[1]
    n_chip = n_tp // 2
    core = j % 2
    partner, xnb, ynb, diag = peers(j)
    barrier = pltpu.get_barrier_semaphore()
    greet = [(lax.rem(i + d, n_ep), j) for d in range(1, n_ep)]
    greet += [(i, lax.rem(j + d, n_tp)) for d in range(1, n_tp)]
    signal_all(barrier, greet)
    loads = []
    for index, (source, target) in enumerate(((wg_hbm, wg), (wu_hbm, wu), (wd_hbm, wd))):
        load = pltpu.make_async_copy(source, target, in_sem.at[index])
        load.start()
        loads.append(load)

    m0, m1, slot = routing(routes_ref)
    weight = jnp.where(m0, weights_ref[0:1, :], 0.0) + jnp.where(m1, weights_ref[1:2, :], 0.0)
    for e in range(n_ep):
        mask = slot_mask(slot, e, capacity)
        pick = jnp.where(mask, 1.0, 0.0).astype(BF16)
        rows = jnp.dot(pick, tok_ref[...], preferred_element_type=F32)
        grads = jnp.dot(pick, go_ref[...], preferred_element_type=F32)
        scale = jnp.sum(jnp.where(mask, weight[e : e + 1, :], 0.0), axis=1, keepdims=True)
        send_buf[e, 0] = rows.astype(BF16)
        send_buf[e, 1] = (grads * scale).astype(BF16)

    def rows_at(e):
        return pl.ds(pl.multiple_of(e * capacity, capacity), capacity)

    def cols_at(t):
        return pl.ds(pl.multiple_of(t * width, width), width)

    def area(src, col):
        return full.at[:, rows_at(src), cols_at(col)]

    area(i, j)[...] = send_buf[i]
    pl.semaphore_wait(barrier, len(greet))

    z_copies = {}
    for d in [1, 3, 2]:
        e = lax.rem(i + d, n_ep)
        z_copies[d] = remote(send_buf.at[e], area(i, j), zs.at[d], zr.at[d], (e, j))
        z_copies[d].start()

    copies = []
    heard = {}

    def push(kind, d, source, target, device):
        copy = remote(source, target, ts.at[kind, d], tr.at[kind, d], (i, device))
        copy.start()
        copies.append(copy)
        heard[kind, d] = copy

    order = [0, 1, 3, 2]
    for step in range(len(order) + 2):
        if step < len(order):
            d = order[step]
            src = lax.rem(i + n_ep - d, n_ep)
            if d > 0:
                z_copies[d].wait_recv()
            mine = area(src, j) if d > 0 else send_buf.at[i]
            push(0, d, mine, area(src, j), xnb)
            push(1, d, mine, area(src, j), ynb)
            push(4, d, mine, area(src, j), partner)
        if 0 < step <= len(order):
            d = order[step - 1]
            src = lax.rem(i + n_ep - d, n_ep)
            heard[0, d].wait_recv()
            half = full.at[0, rows_at(src), cols_at(xnb)]
            push(2, d, half, half, ynb)
            push(5, d, area(src, xnb), area(src, xnb), partner)
            heard[1, d].wait_recv()
            half = full.at[1, rows_at(src), cols_at(ynb)]
            push(3, d, half, half, xnb)
            push(6, d, area(src, ynb), area(src, ynb), partner)
        if step > 1:
            d = order[step - 2]
            src = lax.rem(i + n_ep - d, n_ep)
            for kind in (0, 1):
                heard[2 + kind, d].wait_recv()
                half = full.at[kind, rows_at(src), cols_at(diag)]
                push(7 + kind, d, half, half, partner)
    for d in order:
        for kind in (4, 5, 6, 7, 8):
            heard[kind, d].wait_recv()

    save = pltpu.make_async_copy(full, full_hbm, in_sem.at[3])
    save.start()
    for load in loads:
        load.wait()
    gate = lax.dot_general(full[0], wg[...], NT, preferred_element_type=F32)
    up = lax.dot_general(full[0], wu[...], NT, preferred_element_type=F32)
    dhid = lax.dot_general(full[1], wd[...], NT, preferred_element_type=F32)
    sig = 1.0 / (1.0 + jnp.exp(-gate))
    active = gate * sig
    slope = sig * (1.0 + gate * (1.0 - sig))
    hidden_f = (active * up).astype(BF16).astype(F32)
    dgate_f = dhid * up * slope
    dup_f = dhid * active
    dgate, dup = dgate_f.astype(BF16), dup_f.astype(BF16)

    ring = [2, 1, 3, 0]
    pair = {}
    for q in range(n_chip):
        cols = slice(2 * q * width, 2 * (q + 1) * width)
        back[:, cols] = (
            jnp.dot(dgate, wg[:, cols], preferred_element_type=F32)
            + jnp.dot(dup, wu[:, cols], preferred_element_type=F32)
        ).astype(BF16)
        for d in ring:
            e = lax.rem(i + d, n_ep)
            pair[d, q] = remote(
                back.at[rows_at(e), cols_at(2 * q + 1 - core)],
                pair_in.at[d, q],
                ps.at[d, q],
                pr.at[d, q],
                (i, partner),
            )
            pair[d, q].start()

    route_terms = hidden_f * dhid
    part_out[...] = jnp.zeros_like(part_out)
    for e in range(n_ep):
        block = route_terms[e * capacity : (e + 1) * capacity, :]
        part_out[e : e + 1, 0:capacity] = jnp.sum(block.T, axis=0, keepdims=True)
    part = []
    for d in range(1, n_tp):
        copy = remote(
            part_out, part_in.at[d - 1], qs.at[d - 1], qr.at[d - 1], (i, lax.rem(j + d, n_tp))
        )
        copy.start()
        part.append(copy)

    plane = {}
    for d in ring:
        e = lax.rem(i + d, n_ep)
        for q in range(n_chip):
            pair[d, q].wait_recv()
            mine = back[rows_at(e), cols_at(2 * q + core)].astype(F32)
            chip_sum[d, q] = (mine + pair_in[d, q].astype(F32)).astype(BF16)
        for kind, target in enumerate((diag, xnb, ynb)):
            plane[d, kind] = remote(
                chip_sum.at[d, target // 2],
                plane_in.at[d, kind],
                cs.at[d, kind],
                cr.at[d, kind],
                (i, target),
            )
            plane[d, kind].start()

    lhs_ref[0] = dgate_f.T.astype(BF16)
    lhs_ref[1] = dup_f.T.astype(BF16)
    lhs_ref[2] = hidden_f.T.astype(BF16)
    rows_norm = model_width // 128
    tile = 512
    for index in range(2):
        for n in range(model_width // tile):
            cols = slice(n * tile, (n + 1) * tile)
            grad = jnp.dot(lhs_ref[index], full[0, :, cols], preferred_element_type=F32)
            norm = jnp.sum(grad * grad, axis=0, keepdims=True)
            for q in range(tile // 128):
                row = index * rows_norm + n * (tile // 128) + q
                norm_out[row : row + 1, :] = norm[:, q * 128 : (q + 1) * 128]
    norms = []
    for d in range(1, n_tp):
        copy = remote(
            norm_out, norm_in.at[d - 1], ns.at[d - 1], nr.at[d - 1], (i, lax.rem(j + d, n_tp))
        )
        copy.start()
        norms.append(copy)

    for copy in part:
        copy.wait_recv()
    total = part_out[...]
    for d in range(1, n_tp):
        total = total + part_in[d - 1]
    route_out[...] = total
    route_in[i] = total
    route = []
    for d in range(1, n_ep):
        copy = remote(
            route_out, route_in.at[i], rs.at[d], rr.at[d], (lax.rem(i + d, n_ep), j)
        )
        copy.start()
        route.append(copy)

    returns = []
    for d in ring:
        for kind in range(3):
            plane[d, kind].wait_recv()
        done = (
            chip_sum[d, j // 2].astype(F32)
            + plane_in[d, 0].astype(F32)
            + plane_in[d, 1].astype(F32)
            + plane_in[d, 2].astype(F32)
        ).astype(BF16)
        if d == 0:
            z_in[i] = done
        else:
            z_out[d] = done
            copy = remote(
                z_out.at[d], z_in.at[i], bs.at[d], br.at[d], (lax.rem(i + d, n_ep), j)
            )
            copy.start()
            returns.append(copy)

    for copy in norms:
        copy.wait_recv()
    total = norm_out[...]
    for d in range(1, n_tp):
        total = total + norm_in[d - 1]
    norm_total[...] = total
    for copy in (*route, *returns):
        copy.wait_recv()
    for copy in (
        *z_copies.values(), *copies, *pair.values(), *part, *plane.values(),
        *norms, *route, *returns,
    ):
        copy.wait_send()
    save.wait()


def finish_kernel(
    n_ep, capacity, routes_ref, weights_ref, full_hbm, lhs_ref, z_in, route_in, norm_total,
    gg_hbm, gu_hbm, gd_hbm, gt_ref, gr_ref, gn_ref, un_ref, dn_ref,
    full, gg, gu, gd, in_sem, out_sem,
):
    loads = []
    for index in range(2):
        load = pltpu.make_async_copy(full_hbm.at[index], full.at[index], in_sem.at[index])
        load.start()
        loads.append(load)
    _, hidden_dev, _ = lhs_ref.shape
    model_width = full.shape[2]
    tile = 512
    stores = []
    down_sums = jnp.zeros((hidden_dev, 128), F32)
    for index, (rhs, buf, out) in enumerate(((0, gg, gg_hbm), (0, gu, gu_hbm), (1, gd, gd_hbm))):
        if index != 1:
            loads[rhs].wait()
        for n in range(model_width // tile):
            cols = slice(n * tile, (n + 1) * tile)
            grad = jnp.dot(lhs_ref[index], full[rhs, :, cols], preferred_element_type=F32)
            buf[:, cols] = grad
            store = pltpu.make_async_copy(
                buf.at[:, cols], out.at[:, cols], out_sem.at[index, n]
            )
            store.start()
            stores.append(store)
            if index == 2:
                square = grad * grad
                for q in range(tile // 128):
                    down_sums = down_sums + square[:, q * 128 : (q + 1) * 128]
    dn_ref[...] = jnp.sum(down_sums.T, axis=0, keepdims=True)
    rows_norm = model_width // 128
    for r in range(rows_norm):
        gn_ref[:, r * 128 : (r + 1) * 128] = norm_total[r : r + 1, :]
        un_ref[:, r * 128 : (r + 1) * 128] = norm_total[rows_norm + r : rows_norm + r + 1, :]

    i = lax.axis_index("ep")
    m0, m1, slot = routing(routes_ref)
    acc = jnp.zeros(gt_ref.shape, F32)
    back_route = []
    for e in range(n_ep):
        pick = jnp.where(slot_mask(slot, e, capacity), 1.0, 0.0)
        acc = acc + jnp.dot(pick.T.astype(BF16), z_in[e], preferred_element_type=F32)
        values = route_in[e, pl.ds(i, 1), :][:, 0:capacity]
        back_route.append(
            jnp.dot(
                values, pick, preferred_element_type=F32, precision=lax.Precision.HIGHEST
            )
        )
    gt_ref[...] = acc.astype(BF16)
    for k, m in enumerate((m0, m1)):
        value = jnp.zeros_like(back_route[0])
        for e in range(n_ep):
            value = value + jnp.where(m[e : e + 1, :], back_route[e], 0.0)
        gr_ref[k : k + 1, :] = value / weights_ref[k : k + 1, :]
    for store in stores:
        store.wait()


def per_device_kernels(tokens, routes, route_weights, grad_out, w_gate, w_up, w_down):
    token_count, width = tokens.shape
    _, hidden_dev, model_width = w_gate.shape
    n_ep, n_tp = lax.axis_size("ep"), lax.axis_size("tp")
    n_chip = n_tp // 2
    capacity = min(3 * token_count // n_ep, token_count // 2)
    rows = n_ep * capacity
    block = (capacity, width)
    norm_rows = 2 * (model_width // 128)
    routes_t, weights_t = routes.T, route_weights.T
    dma = pltpu.SemaphoreType.DMA
    full, lhs, z_in, route_in, norm_total = pl.pallas_call(
        functools.partial(step_kernel, n_ep, n_tp, capacity),
        name="step",
        out_shape=(
            jax.ShapeDtypeStruct((2, rows, model_width), BF16),
            jax.ShapeDtypeStruct((3, hidden_dev, rows), BF16),
            jax.ShapeDtypeStruct((n_ep, *block), BF16),
            jax.ShapeDtypeStruct((n_ep, 8, 128), F32),
            jax.ShapeDtypeStruct((norm_rows, 128), F32),
        ),
        in_specs=[VMEM] * 4 + [ANY] * 3,
        out_specs=(ANY, VMEM, VMEM, VMEM, VMEM),
        scratch_shapes=[
            pltpu.VMEM((2, rows, model_width), BF16),
            pltpu.VMEM((n_ep, 2, *block), BF16),
            *[pltpu.VMEM((hidden_dev, model_width), BF16)] * 3,
            pltpu.VMEM((rows, model_width), BF16),
            pltpu.VMEM((n_ep, n_chip, *block), BF16),
            pltpu.VMEM((n_ep, n_chip, *block), BF16),
            pltpu.VMEM((n_ep, 3, *block), BF16),
            pltpu.VMEM((n_ep, *block), BF16),
            pltpu.VMEM((8, 128), F32),
            pltpu.VMEM((n_tp - 1, 8, 128), F32),
            pltpu.VMEM((8, 128), F32),
            pltpu.VMEM((norm_rows, 128), F32),
            pltpu.VMEM((n_tp - 1, norm_rows, 128), F32),
            dma((4,)),
            *[dma((n_ep,))] * 2,
            *[dma((9, n_ep))] * 2,
            *[dma((n_ep, n_chip))] * 2,
            *[dma((n_ep, 3))] * 2,
            *[dma((n_tp - 1,))] * 2,
            *[dma((n_ep,))] * 2,
            *[dma((n_tp - 1,))] * 2,
            *[dma((n_ep,))] * 2,
        ],
        compiler_params=pltpu.CompilerParams(collective_id=0, has_side_effects=True),
    )(routes_t, weights_t, tokens, grad_out, w_gate[0], w_up[0], w_down[0])

    grad_shape = jax.ShapeDtypeStruct((hidden_dev, model_width), F32)
    norm_shape = jax.ShapeDtypeStruct((1, model_width), F32)
    grad_gate, grad_up, grad_down, grad_tokens, grad_route, gate_norms, up_norms, down_norms = (
        pl.pallas_call(
            functools.partial(finish_kernel, n_ep, capacity),
            name="finish",
            out_shape=(
                *[grad_shape] * 3,
                jax.ShapeDtypeStruct((token_count, width), BF16),
                jax.ShapeDtypeStruct((2, token_count), F32),
                *[norm_shape] * 2,
                jax.ShapeDtypeStruct((1, hidden_dev), F32),
            ),
            in_specs=[VMEM, VMEM, ANY, VMEM, VMEM, VMEM, VMEM],
            out_specs=(*[ANY] * 3, *[VMEM] * 5),
            scratch_shapes=[
                pltpu.VMEM((2, rows, model_width), BF16),
                *[pltpu.VMEM((hidden_dev, model_width), F32)] * 3,
                dma((2,)),
                dma((3, model_width // 512)),
            ],
        )(routes_t, weights_t, full, lhs, z_in, route_in, norm_total)
    )
    return (
        grad_tokens,
        grad_route.T,
        grad_gate[None],
        grad_up[None],
        grad_down[None],
        gate_norms,
        up_norms,
        down_norms,
    )


def silu_parts(pre_act):
    sigmoid_val = jax.nn.sigmoid(pre_act)
    return (pre_act * sigmoid_val, sigmoid_val * (1.0 + pre_act * (1.0 - sigmoid_val)))


def per_device(tokens, routes, route_weights, grad_out, w_gate, w_up, w_down):
    token_count, feature_dev = tokens.shape
    experts_dev, hidden_dev, model_width = w_gate.shape
    ep_size = lax.axis_size("ep")
    expert_total = experts_dev * ep_size
    capacity = min(3 * token_count // expert_total, token_count // 2)
    slot_count = expert_total * capacity
    row_count = ep_size * capacity
    flat_ids = routes.reshape(-1)
    pair_count = flat_ids.shape[0]
    one_hot = (flat_ids[:, None] == jnp.arange(expert_total, dtype=jnp.int32)[None, :]).astype(
        jnp.bfloat16
    )
    lower = (
        jnp.arange(pair_count, dtype=jnp.int32)[:, None]
        > jnp.arange(pair_count, dtype=jnp.int32)[None, :]
    ).astype(jnp.bfloat16)
    earlier = jnp.dot(lower, one_hot, preferred_element_type=jnp.float32)
    slot_ids = jnp.sum(earlier * one_hot.astype(jnp.float32), axis=1).astype(jnp.int32)
    position = flat_ids % experts_dev * row_count + flat_ids // experts_dev * capacity + slot_ids
    dispatch = (position[None, :] == jnp.arange(slot_count, dtype=jnp.int32)[:, None]).astype(
        jnp.bfloat16
    )
    weight_flat = route_weights.reshape(-1)
    token_rows = jnp.repeat(tokens, 2, axis=0)
    scaled = (weight_flat[:, None] * jnp.repeat(grad_out, 2, axis=0).astype(jnp.float32)).astype(
        jnp.bfloat16
    )
    send_shape = (experts_dev, ep_size, capacity, feature_dev)
    x_send = (
        jnp.dot(dispatch, token_rows, preferred_element_type=jnp.float32)
        .astype(jnp.bfloat16)
        .reshape(send_shape)
    )
    s_send = (
        jnp.dot(dispatch, scaled, preferred_element_type=jnp.float32)
        .astype(jnp.bfloat16)
        .reshape(send_shape)
    )
    x_recv, s_recv = (
        lax.all_to_all(x_send, "ep", split_axis=1, concat_axis=1, tiled=True),
        lax.all_to_all(s_send, "ep", split_axis=1, concat_axis=1, tiled=True),
    )
    x_full, s_full = (
        lax.all_gather(x_recv, "tp", axis=3, tiled=True),
        lax.all_gather(s_recv, "tp", axis=3, tiled=True),
    )
    x_rows = x_full.reshape(experts_dev, row_count, model_width)
    s_rows = s_full.reshape(experts_dev, row_count, model_width)
    gate = jnp.einsum("erd,efd->erf", x_rows, w_gate, preferred_element_type=jnp.float32)
    up = jnp.einsum("erd,efd->erf", x_rows, w_up, preferred_element_type=jnp.float32)
    dhid = jnp.einsum("erd,efd->erf", s_rows, w_down, preferred_element_type=jnp.float32)
    active, slope = silu_parts(gate)
    hidden = (active * up).astype(jnp.bfloat16)
    partial_value = jnp.sum(hidden.astype(jnp.float32) * dhid, axis=2)
    dgate = (dhid * up * slope).astype(jnp.bfloat16)
    dup = (dhid * active).astype(jnp.bfloat16)
    grad_gate = jnp.einsum("erf,erd->efd", dgate, x_rows, preferred_element_type=jnp.float32)
    grad_up = jnp.einsum("erf,erd->efd", dup, x_rows, preferred_element_type=jnp.float32)
    grad_down = jnp.einsum("erf,erd->efd", hidden, s_rows, preferred_element_type=jnp.float32)
    back_terms = jnp.einsum("erf,efd->erd", dgate, w_gate, preferred_element_type=jnp.float32)
    back_terms = back_terms + jnp.einsum(
        "erf,efd->erd", dup, w_up, preferred_element_type=jnp.float32
    )
    back_terms = back_terms.reshape(experts_dev, ep_size, capacity, model_width)
    gate_norms = jnp.sum(grad_gate * grad_gate, axis=1)
    up_norms = jnp.sum(grad_up * grad_up, axis=1)
    down_norms = jnp.sum(grad_down * grad_down, axis=2)
    partial_value, gate_norms, up_norms = lax.psum((partial_value, gate_norms, up_norms), "tp")
    partial_sent = partial_value.reshape(experts_dev, ep_size, capacity)
    dtok_mine = lax.psum_scatter(
        back_terms.astype(jnp.bfloat16), "tp", scatter_dimension=3, tiled=True
    ).astype(jnp.float32)
    returned, partial_back = (
        lax.all_to_all(
            dtok_mine.astype(jnp.bfloat16), "ep", split_axis=1, concat_axis=1, tiled=True
        ).astype(dtok_mine.dtype),
        lax.all_to_all(
            partial_sent.astype(jnp.bfloat16), "ep", split_axis=1, concat_axis=1, tiled=True
        ).astype(partial_sent.dtype),
    )
    slot_rows = jnp.take(returned.reshape(slot_count, feature_dev), position, axis=0)
    grad_tokens = jnp.sum(slot_rows.reshape(token_count, 2, feature_dev), axis=1).astype(
        jnp.bfloat16
    )
    slot_partial = jnp.take(partial_back.reshape(slot_count), position, axis=0)
    grad_route = (slot_partial / weight_flat).reshape(token_count, 2)
    return (
        grad_tokens,
        grad_route,
        grad_gate,
        grad_up,
        grad_down,
        gate_norms,
        up_norms,
        down_norms,
    )


def solution(mesh):
    in_specs = (
        P("ep", "tp"),
        P("ep", None),
        P("ep", None),
        P("ep", "tp"),
        P("ep", "tp", None),
        P("ep", "tp", None),
        P("ep", "tp", None),
    )
    out_specs = (
        P("ep", "tp"),
        P("ep", None),
        P("ep", "tp", None),
        P("ep", "tp", None),
        P("ep", "tp", None),
        P("ep", None),
        P("ep", None),
        P("ep", "tp"),
    )
    fits = mesh.shape["tp"] == 8 and mesh.shape["ep"] == 4
    return jax.shard_map(
        per_device_kernels if fits else per_device, mesh=mesh, in_specs=in_specs, out_specs=out_specs, check_vma=False
    )
```
